32 devices in a mesh: ep: 8 (over z, x), tp: 4 (over y, core).
Axes of the slice: x: 2, y: 2, z: 4, core: 2. Of those that a mesh axis runs over, the one named last changes fastest.
Arguments:
- queries: bfloat16 [4096, 1024], P('ep', 'tp'), may hold values from -6 to 6
- key_input: bfloat16 [4096, 256], P('ep'), may hold values from -6 to 6
- value_input: bfloat16 [4096, 256], P('ep'), may hold values from -6 to 6
- query_gain: float32 [64], replicated, may hold values from 0.1 to 1.9
- key_gain: float32 [64], replicated, may hold values from 0.1 to 1.9
- mix_out_weight: bfloat16 [1024, 2048], P('tp'), may hold values from -0.1875 to 0.1875
- expert_input: bfloat16 [1280, 2048], P('ep'), may hold values from -6 to 6
- ffn_gain: float32 [2048], replicated, may hold values from 0.1 to 1.9
- routes: int32 [1280, 2], P('ep'), may hold values from 0 to 7, all different within a row; in each aligned block of 160 rows (0 to 159, 160 to 319, ...) at most 60 rows name the same one
- route_scores: float32 [1280, 2], P('ep'), may hold values from 0.1 to 1
- gate_weight: bfloat16 [8, 2048, 4096], P('ep', None, 'tp'), may hold values from -0.125 to 0.125
- up_weight: bfloat16 [8, 2048, 4096], P('ep', None, 'tp'), may hold values from -0.125 to 0.125
- down_weight: bfloat16 [8, 4096, 2048], P('ep', 'tp'), may hold values from -0.09375 to 0.09375
Outputs:
- mixed_rows: bfloat16 [4096, 2048], P(('ep', 'tp'))
- expert_out: bfloat16 [1280, 2048], P('ep', 'tp')
The draws below stay inside these ranges and needn't reach their ends.
Inputs may be any that keep to these rules, and one draw needn't show every extreme that they name: `routes`: each row names 2 different experts. Within the rows of one index of ep (aligned blocks of 160 rows) no expert is named by more than 60 rows, and in every draw some expert is named by exactly 60 rows of some block.
All inputs are finite; a program needn't handle non-finite values.
Results may differ from the reference program's by a relative error of at most 0.019.
The reference program's roundings to bfloat16 on the way count: a program that leaves them out, or rounds other values in their place, can miss the bound.
Values may be sent and summed in bfloat16 or wider, within the bound.
A program may use at most 64 MiB of HBM per device.

```python
import math
import jax
import jax.numpy as jnp
import numpy as np
from jax import lax

D = 2048
HEADS = 16
KV_HEADS = 4
HD = 64
GRID_W = 64
FF = 4096
TOPK = 2
TOK2 = 160
EXPERTS = 8
CAP = 60
TOKENS1 = 4096
TOKENS2 = 1280
N_EP = 8
N_TP = 4


def block_levels(rng, dims, shards, least, top_value):
    loudness = 1.0
    for dim, parts in shards:
        heights = jax.random.uniform(jax.random.fold_in(jax.random.fold_in(rng, 6), dim), (parts,), jnp.float32, least / len(shards), top_value / len(shards))
        loudness = loudness * jnp.repeat(jnp.exp(heights), dims[dim] // parts).reshape((-1,) + (1,) * (len(dims) - 1 - dim))
    return loudness


def routed_block(stream_key, own, number, rows, number_of, top, most, skew):
    order = jax.random.permutation(stream_key, number_of)
    crowded, usual = portions_of(number_of, rows * top, most, skew, True), portions_of(number_of, rows * top, most, skew, False)
    places = jnp.arange(number_of)

    def named(tallies, rotation):
        used = int((tallies > 0).sum())
        fixed = max(1, used // 4)
        passed = fixed + (places - fixed + rotation * (used - fixed)) % max(1, number_of - fixed)
        return jnp.zeros((number_of,), jnp.int32).at[order[jnp.where(places < fixed, places, passed)]].set(jnp.asarray(tallies, jnp.int32))

    tallies = jnp.where(number % 4 == 0, named(crowded, number // 4), named(usual, number - number // 4 - 1))
    mixed = jax.random.permutation(jax.random.fold_in(own, 3), number_of)
    donor, taker = mixed[0:number_of // 2 * 2:2], mixed[1:number_of // 2 * 2:2]
    margin = jnp.minimum(tallies[donor] - 1, most - tallies[taker]) // 2
    margin = jnp.where((donor == order[0]) | (taker == order[0]) | (tallies[taker] == 0), 0, jnp.maximum(margin, 0))
    passed = jax.random.randint(jax.random.fold_in(own, 4), (number_of // 2,), 0, 1 << 20) % (margin + 1)
    tallies = tallies.at[donor].add(-passed).at[taker].add(passed)
    items = jnp.searchsorted(jnp.cumsum(tallies), jnp.arange(rows * top), side="right").astype(jnp.int32)
    listing = items.reshape(top, rows).T
    listing = listing[jax.random.permutation(jax.random.fold_in(own, 1), rows)]
    rotation = jax.random.randint(jax.random.fold_in(own, 2), (rows, 1), 0, top)
    return jnp.take_along_axis(listing, (jnp.arange(top)[None, :] + rotation) % top, axis=1)


def portions_of(count, total, bound, skew, full):
    loads = [(1 << 20) // math.isqrt(rank ** skew) + 1 for rank in range(1, count + 1)]
    largest = bound if full else min(bound, max(-(-total // count), total * loads[0] // sum(loads)))
    least = 1 if total - largest >= count - 1 else 0
    given, spare = [largest] + [least] * (count - 1), total - largest - least * (count - 1)
    while spare > 0:
        movable = [i for i in range(1, count) if given[i] < largest] or [i for i in range(1, count) if given[i] < bound]
        whole, budget = sum([loads[i] for i in movable]), spare
        for i in movable:
            more = min(bound - given[i], max(1, budget * loads[i] // whole), spare)
            given[i] = given[i] + more
            spare = spare - more
    return np.array(given)


def noise(key, extent, deviation, bound, cuts=(), kind=jnp.bfloat16):
    factor_of = block_levels(key, extent, cuts, -0.22, 0.18) if cuts else 1.0
    array = jax.random.normal(key, extent, jnp.float32) * deviation * factor_of
    return jnp.minimum(jnp.maximum(array, -bound), bound).astype(kind)


def setup_inputs(seed: int = 0) -> dict:
    streams_of = jax.random.split(jax.random.key(seed), 14)
    queries = noise(streams_of[0], (TOKENS1, HEADS * HD), 1.0, 6.0, ((0, 8), (1, 4)))
    key_input = noise(streams_of[1], (TOKENS1, KV_HEADS * HD), 1.0, 6.0, ((0, 8),))
    value_input = noise(streams_of[2], (TOKENS1, KV_HEADS * HD), 1.0, 6.0, ((0, 8),))
    query_gain = jnp.clip(1.0 + 0.18 * jax.random.normal(streams_of[3], (HD,), jnp.float32), 0.1, 1.9)
    key_gain = jnp.clip(1.0 + 0.18 * jax.random.normal(streams_of[4], (HD,), jnp.float32), 0.1, 1.9)
    mix_out_weight = noise(streams_of[5], (HEADS * HD, D), (HEADS * HD) ** -0.5, 0.1875, ((0, 4),))
    expert_input = noise(streams_of[6], (TOKENS2, D), 1.0, 6.0, ((0, 8),))
    ffn_gain = jnp.clip(1.0 + 0.18 * jax.random.normal(streams_of[7], (D,), jnp.float32), 0.1, 1.9)
    routes_keys = jax.random.split(jax.random.fold_in(streams_of[8], 1), TOKENS2 // TOK2)
    routes_turns = jax.random.permutation(jax.random.fold_in(streams_of[8], 3), TOKENS2 // TOK2)
    routes = jax.vmap(lambda own, number: routed_block(jax.random.fold_in(streams_of[8], 2), own, number, TOK2, EXPERTS, TOPK, CAP, 2))(routes_keys, routes_turns).reshape((TOKENS2, TOPK))
    route_scores = jnp.clip(jnp.exp(math.log(1.0) - 2.3025851 * jax.random.uniform(streams_of[9], (TOKENS2, TOPK), jnp.float32) ** block_levels(streams_of[9], (TOKENS2, TOPK), ((0, 8),), -0.2, 0.2)), 0.1, 1.0)
    gate_weight = noise(streams_of[10], (EXPERTS, D, FF), D ** -0.5, 0.125, ((0, 8), (2, 4)))
    up_weight = noise(streams_of[11], (EXPERTS, D, FF), D ** -0.5, 0.125, ((0, 8), (2, 4)))
    down_weight = noise(streams_of[12], (EXPERTS, FF, D), FF ** -0.5, 0.09375, ((0, 8), (1, 4)))
    return dict(queries=queries, key_input=key_input, value_input=value_input, query_gain=query_gain, key_gain=key_gain, mix_out_weight=mix_out_weight, expert_input=expert_input, ffn_gain=ffn_gain, routes=routes, route_scores=route_scores, gate_weight=gate_weight, up_weight=up_weight, down_weight=down_weight)


EPSILON = 1e-06
ROPE_BASE = 10000.0

def rotate_half(portion, cos_table, sin_table):
    front_half, back_half = jnp.split(portion, 2, axis=-1)
    cos_table = cos_table[:, None, :]
    sin_table = sin_table[:, None, :]
    return jnp.concatenate([front_half * cos_table - back_half * sin_table, back_half * cos_table + front_half * sin_table], axis=-1)

def prepare(source, channel_gain, positions):
    token_count = source.shape[0]
    values_f = source.astype(jnp.float32).reshape(token_count, -1, HD)
    normed = values_f * lax.rsqrt(lax.optimization_barrier(jnp.mean(values_f * values_f, axis=-1, keepdims=True)) + EPSILON) * channel_gain
    quarter = HD // 4
    inverse = ROPE_BASE ** (-jnp.arange(quarter, dtype=jnp.float32) / quarter)
    row_angle = (positions // GRID_W).astype(jnp.float32)[:, None] * inverse[None, :]
    col_angle = (positions % GRID_W).astype(jnp.float32)[:, None] * inverse[None, :]
    half_width = HD // 2
    turned = jnp.concatenate([rotate_half(normed[..., :half_width], jnp.cos(row_angle), jnp.sin(row_angle)), rotate_half(normed[..., half_width:], jnp.cos(col_angle), jnp.sin(col_angle))], axis=-1)
    return turned.reshape(token_count, -1).astype(jnp.bfloat16)

def attend_head(head_args):
    query_head, key_head, value_head = head_args
    length = query_head.shape[0]
    key_span = math.gcd(length, 512)
    query_blocks = query_head.reshape(length // key_span, key_span, HD)

    def one_block(query_block):
        scores = jnp.dot(query_block, key_head.T, preferred_element_type=jnp.float32) * HD ** (-0.5)
        weights = jnp.exp(scores)
        weighted = jnp.dot(weights.astype(jnp.bfloat16), value_head, preferred_element_type=jnp.float32)
        return (weighted / lax.optimization_barrier(jnp.sum(weights, axis=-1, keepdims=True))).astype(jnp.bfloat16)
    return lax.map(one_block, query_blocks).reshape(length, HD)

def reference(queries, key_input, value_input, query_gain, key_gain, mix_out_weight, expert_input, ffn_gain, routes, route_scores, gate_weight, up_weight, down_weight):
    length = queries.shape[0]
    positions = jnp.arange(length, dtype=jnp.int32)
    group_size = HEADS // KV_HEADS
    q_rot = prepare(queries, query_gain, positions).reshape(length, HEADS, HD).transpose(1, 0, 2)
    k_rot = prepare(key_input, key_gain, positions).reshape(length, KV_HEADS, HD).transpose(1, 0, 2)
    v_heads = value_input.reshape(length, KV_HEADS, HD).transpose(1, 0, 2)
    attended = lax.map(attend_head, (q_rot, jnp.repeat(k_rot, group_size, axis=0), jnp.repeat(v_heads, group_size, axis=0)))
    attended = attended.transpose(1, 0, 2).reshape(length, HEADS * HD)
    col_width = HEADS * HD // N_TP

    def add_group(running_sum, group_index):
        start_col = (group_index * col_width).astype(jnp.int32)
        columns = lax.dynamic_slice_in_dim(attended, start_col, col_width, 1)
        weight_rows = lax.dynamic_slice_in_dim(mix_out_weight, start_col, col_width, 0)
        portion = jnp.dot(columns, weight_rows, preferred_element_type=jnp.float32).astype(jnp.bfloat16)
        portion = lax.optimization_barrier(portion)
        return (running_sum + portion.astype(jnp.float32), None)
    mixed_sum, _ = lax.scan(add_group, jnp.zeros((length, D), jnp.float32), jnp.arange(N_TP, dtype=jnp.int32))
    mixed_rows = mixed_sum.astype(jnp.bfloat16)
    tokens = expert_input.shape[0]
    flat_routes = routes.reshape(N_EP, TOK2 * TOPK)
    hit_table = (flat_routes[:, :, None] == jnp.arange(EXPERTS, dtype=jnp.int32)[None, None, :]).astype(jnp.int32)
    position = lax.optimization_barrier(jnp.sum((jnp.cumsum(hit_table, axis=1) - hit_table) * hit_table, axis=-1))
    per_expert = N_EP * CAP
    slot_index = flat_routes * per_expert + jnp.arange(N_EP, dtype=jnp.int32)[:, None] * CAP + position
    slot_index = slot_index.reshape(-1).astype(jnp.int32)
    pair_token = jnp.arange(tokens * TOPK, dtype=jnp.int32) // TOPK
    owner_row = jnp.full((EXPERTS * per_expert,), tokens, jnp.int32).at[slot_index].set(pair_token)
    padded = jnp.concatenate([expert_input, jnp.zeros((1, D), jnp.bfloat16)], axis=0)
    buffers = padded[owner_row].reshape(EXPERTS, per_expert, D)
    ff_width = FF // N_TP

    def run_expert(expert_args):
        slot_rows, w_gate, w_up, w_down = expert_args
        values_f = slot_rows.astype(jnp.float32)
        row_scale = lax.rsqrt(lax.optimization_barrier(jnp.mean(values_f * values_f, axis=-1, keepdims=True)) + EPSILON)
        scaled = (values_f * ffn_gain).astype(jnp.bfloat16)
        gate_pre = row_scale * jnp.dot(scaled, w_gate, preferred_element_type=jnp.float32)
        up_pre = row_scale * jnp.dot(scaled, w_up, preferred_element_type=jnp.float32)
        hidden = (jax.nn.silu(gate_pre) * up_pre).astype(jnp.bfloat16)
        running_sum = jnp.zeros((per_expert, D), jnp.float32)
        for group_index in range(N_TP):
            lower = group_index * ff_width
            portion = jnp.dot(hidden[:, lower:lower + ff_width], w_down[lower:lower + ff_width], preferred_element_type=jnp.float32).astype(jnp.bfloat16)
            running_sum = running_sum + lax.optimization_barrier(portion).astype(jnp.float32)
        return running_sum.astype(jnp.bfloat16)
    pair_rows = lax.map(run_expert, (buffers, gate_weight, up_weight, down_weight)).reshape(-1, D)
    route_weight = route_scores / lax.optimization_barrier(jnp.sum(route_scores, axis=-1, keepdims=True))
    picked = pair_rows[slot_index].astype(jnp.float32).reshape(tokens, TOPK, D)
    expert_out = lax.optimization_barrier(jnp.sum(picked * route_weight[:, :, None], axis=1)).astype(jnp.bfloat16)
    return (mixed_rows, expert_out)
```

```python
import functools
import math

import jax
import jax.numpy as jnp
from jax import lax
from jax.experimental import pallas as pl
from jax.experimental.pallas import tpu as pltpu
from jax.sharding import PartitionSpec as P

HEADS = 16
KV_HEADS = 4
HD = 64
GRID_W = 64
EPSILON = 1e-06
ROPE_BASE = 10000.0
MESH = pl.DeviceIdType.MESH
LANES = 128
BF = jnp.bfloat16
F32 = jnp.float32


def prep(values, gain, cos_table, sin_table):
    width = values.shape[1]
    squares = values * values
    high = squares.astype(BF)
    low = (squares - high.astype(F32)).astype(BF)
    rows = lax.broadcasted_iota(jnp.int32, (width, width), 0) // HD
    cols = lax.broadcasted_iota(jnp.int32, (width, width), 1) // HD
    same = jnp.where(rows == cols, 1.0, 0.0).astype(BF)
    total = jnp.dot(high, same, preferred_element_type=F32) + jnp.dot(
        low, same, preferred_element_type=F32
    )
    normed = values * lax.rsqrt(total * (1.0 / HD) + EPSILON) * gain
    lane = lax.broadcasted_iota(jnp.int32, normed.shape, 1)
    quarter = HD // 4
    partner = jnp.where(
        lane % (2 * quarter) < quarter,
        pltpu.roll(normed, width - quarter, 1),
        pltpu.roll(normed, quarter, 1),
    )
    return normed * cos_table + partner * sin_table


def kernel(
    n_ep, n_tp, heads, model_width,
    q_ref, kv_ref, qg_ref, kg_ref, cos_ref, sin_ref, wmix_ref, x_ref, gain_ref, routes_ref,
    scores_ref, wg_ref, wu_ref, wd_ref,
    mixed_ref, out_ref,
    kv_buf, q_buf, x_out, x_buf, scaled, hid, wg, wu, wd, wmix, dp_buf, ep_in, es_buf, ey_in,
    ret_out, ret_in, mp_out, mp_in, ms_out, my_in, own_mix,
    w_sem, kv_s, kv_r, di_s, di_r, dy_s, dy_r, dc_s, dc_r, ep_s, ep_r, ey_s, ey_r, rt_s, rt_r,
    mp_s, mp_r, my_s, my_r,
):
    n_y = n_tp // 2
    me = lax.axis_index("ep")
    tp = lax.axis_index("tp")
    my_y, core = tp // 2, tp % 2
    mate = my_y * 2 + 1 - core
    rows = kv_ref.shape[0]
    slots_per = x_buf.shape[2]
    slots = n_ep * slots_per
    col_w = x_buf.shape[3]
    tokens = x_ref.shape[0]

    def y_peer(j):
        return (my_y + j) % n_y

    loads = [
        pltpu.make_async_copy(src, dst, w_sem.at[i])
        for i, (src, dst) in enumerate(
            ((wg_ref.at[0], wg), (wu_ref.at[0], wu), (wd_ref.at[0], wd), (wmix_ref, wmix))
        )
    ]
    for load in loads:
        load.start()

    barrier = pltpu.get_barrier_semaphore()

    def greet(o, carry):
        pl.semaphore_signal(barrier, inc=1, device_id=((me + o) % n_ep, tp), device_id_type=MESH)
        return carry

    lax.fori_loop(1, n_ep, greet, 0)
    for j in range(1, n_y):
        pl.semaphore_signal(
            barrier, inc=1, device_id=(me, y_peer(j) * 2 + core), device_id_type=MESH
        )
    pl.semaphore_signal(barrier, inc=1, device_id=(me, mate), device_id_type=MESH)

    expert_row = lax.broadcasted_iota(jnp.int32, (n_ep, tokens), 0)
    first = jnp.where(expert_row == routes_ref[0:1, :], 1.0, 0.0)
    second = jnp.where(expert_row == routes_ref[1:2, :], 1.0, 0.0)
    earlier = jnp.where(
        lax.broadcasted_iota(jnp.int32, (tokens, tokens), 0)
        < lax.broadcasted_iota(jnp.int32, (tokens, tokens), 1),
        1.0,
        0.0,
    ).astype(BF)
    before = jnp.dot((first + second).astype(BF), earlier, preferred_element_type=F32)
    place = before + expert_row.astype(F32) * slots_per
    slot_a = jnp.sum(first * place, axis=0, keepdims=True).astype(jnp.int32)
    slot_b = jnp.sum(second * place, axis=0, keepdims=True).astype(jnp.int32)
    slot_row = lax.broadcasted_iota(jnp.int32, (slots, tokens), 0)
    pick_a = jnp.where(slot_row == slot_a, 1.0, 0.0).astype(BF)
    pick_b = jnp.where(slot_row == slot_b, 1.0, 0.0).astype(BF)
    sent = jnp.dot(pick_a + pick_b, x_ref[...], preferred_element_type=F32).astype(BF)
    x_out[...] = sent.reshape(x_out.shape)
    x_buf[tp, me] = x_out[me]

    pl.semaphore_wait(barrier, n_ep - 1 + n_y)

    def disp(peer):
        return pltpu.make_async_remote_copy(
            x_out.at[peer], x_buf.at[tp, me], di_s.at[peer], di_r.at[me],
            device_id=(peer, tp), device_id_type=MESH,
        )

    def disp_in(source):
        return pltpu.make_async_remote_copy(
            x_out.at[source], x_buf.at[tp, source], di_s.at[source], di_r.at[source],
            device_id=(source, tp), device_id_type=MESH,
        )

    def kv_copy(peer, origin):
        return pltpu.make_async_remote_copy(
            kv_buf.at[origin], kv_buf.at[origin], kv_s.at[peer], kv_r.at[origin],
            device_id=(peer, tp), device_id_type=MESH,
        )

    def over_y(j, source, owner):
        return pltpu.make_async_remote_copy(
            x_buf.at[owner * 2 + core, source], x_buf.at[owner * 2 + core, source],
            dy_s.at[y_peer(j), source], dy_r.at[owner, source],
            device_id=(me, y_peer(j) * 2 + core), device_id_type=MESH,
        )

    def start_disp(o, carry):
        disp((me + o) % n_ep).start()
        return carry

    lax.fori_loop(1, n_ep, start_disp, 0)
    for j in range(1, n_y):
        over_y(j, me, my_y).start()

    own = kv_ref[...].astype(F32)
    turned = prep(own, kg_ref[...], cos_ref[...], sin_ref[...])
    lane = lax.broadcasted_iota(jnp.int32, own.shape, 1)
    kv_buf[me] = jnp.where(lane < HD, turned, own).astype(BF)

    def start_kv(o, carry):
        kv_copy((me + o) % n_ep, me).start()
        return carry

    lax.fori_loop(1, n_ep, start_kv, 0)

    for tile in range(q_ref.shape[1] // LANES):
        q_tile = prep(
            q_ref[:, tile * LANES:(tile + 1) * LANES].astype(F32),
            qg_ref[...], cos_ref[...], sin_ref[...],
        )
        q_lane = lax.broadcasted_iota(jnp.int32, q_tile.shape, 1)
        for part in range(2):
            head = tile * 2 + part
            if head < heads:
                moved = q_tile if part == 0 else pltpu.roll(q_tile, HD, 1)
                q_buf[head] = jnp.where(q_lane < HD, moved, 0.0).astype(BF)

    def forward(o, carry):
        source = (me + n_ep - o) % n_ep
        disp_in(source).wait_recv()
        for j in range(1, n_y):
            over_y(j, source, my_y).start()
        return carry

    lax.fori_loop(1, n_ep, forward, 0)

    def to_mate(owner, mine):
        quarter = owner * 2 + mine
        return pltpu.make_async_remote_copy(
            x_buf.at[quarter], x_buf.at[quarter], dc_s.at[owner], dc_r.at[owner],
            device_id=(me, mate), device_id_type=MESH,
        )

    to_mate(my_y, core).start()
    for j in range(1, n_y):
        owner = y_peer(j)

        def arrived(source, carry):
            over_y(j, source, owner).wait_recv()
            return carry

        lax.fori_loop(0, n_ep, arrived, 0)
        to_mate(owner, core).start()
    for j in range(n_y):
        to_mate(y_peer(j), 1 - core).wait_recv()

    power = jnp.zeros((slots, 1), F32)
    for q in range(n_tp):
        x_q = x_buf[q].reshape(slots, col_w).astype(F32)
        power = power + jnp.sum(x_q * x_q, axis=1, keepdims=True)
        scaled[:, q * col_w:(q + 1) * col_w] = (
            x_q * gain_ref[:, q * col_w:(q + 1) * col_w]
        ).astype(BF)
    row_scale = lax.rsqrt(power * (1.0 / model_width) + EPSILON)
    loads[0].wait()
    loads[1].wait()
    hidden_w = wg.shape[1]
    tile_w = math.gcd(hidden_w, 256)

    def hidden_tile(i, carry):
        cols = pl.ds(pl.multiple_of(i * tile_w, tile_w), tile_w)
        gate = row_scale * jnp.dot(scaled[...], wg[:, cols], preferred_element_type=F32)
        up = row_scale * jnp.dot(scaled[...], wu[:, cols], preferred_element_type=F32)
        hid[:, cols] = (gate / (1.0 + jnp.exp(-gate)) * up).astype(BF)
        return carry

    lax.fori_loop(0, hidden_w // tile_w, hidden_tile, 0)
    loads[2].wait()
    for q in range(n_tp):
        dp_buf[q] = jnp.dot(
            hid[...], wd[:, q * col_w:(q + 1) * col_w], preferred_element_type=F32
        ).astype(BF)

    def expert_mate(owner, side):
        return pltpu.make_async_remote_copy(
            dp_buf.at[owner * 2 + side], ep_in.at[owner], ep_s.at[owner], ep_r.at[owner],
            device_id=(me, mate), device_id_type=MESH,
        )

    def expert_y(j):
        return pltpu.make_async_remote_copy(
            es_buf.at[y_peer(j)], ey_in.at[my_y], ey_s.at[y_peer(j)], ey_r.at[my_y],
            device_id=(me, y_peer(j) * 2 + core), device_id_type=MESH,
        )

    def expert_y_in(j):
        return pltpu.make_async_remote_copy(
            es_buf.at[y_peer(j)], ey_in.at[y_peer(j)], ey_s.at[y_peer(j)], ey_r.at[y_peer(j)],
            device_id=(me, y_peer(j) * 2 + core), device_id_type=MESH,
        )

    for j in range(n_y):
        expert_mate(y_peer((j + 1) % n_y), 1 - core).start()

    def kv_wait(o, carry):
        source = (me + n_ep - o) % n_ep
        kv_copy(source, source).wait_recv()
        return carry

    lax.fori_loop(1, n_ep, kv_wait, 0)

    def mate_sum(j):
        owner = y_peer(j)
        expert_mate(owner, core).wait_recv()
        return dp_buf[owner * 2 + core].astype(F32) + ep_in[owner].astype(F32)

    for j in range(1, n_y):
        es_buf[y_peer(j)] = mate_sum(j).astype(BF)
        expert_y(j).start()

    def ret(peer, origin):
        return pltpu.make_async_remote_copy(
            ret_out.at[peer], ret_in.at[origin], rt_s.at[peer], rt_r.at[origin],
            device_id=(peer, tp), device_id_type=MESH,
        )

    def return_rows():
        total = mate_sum(0)
        for j in range(1, n_y):
            expert_y_in(j).wait_recv()
            total = total + ey_in[y_peer(j)].astype(F32)
        ret_out[...] = total.astype(BF).reshape(ret_out.shape)
        ret_in[me] = ret_out[me]

        def start_ret(o, carry):
            ret((me + o) % n_ep, me).start()
            return carry

        lax.fori_loop(1, n_ep, start_ret, 0)

    piece = rows // n_y
    half = piece // 2
    factor = HD ** (-0.5) * math.log2(math.e)

    def mix_mate(owner, side):
        return pltpu.make_async_remote_copy(
            mp_out.at[owner, side], mp_in.at[owner], mp_s.at[owner], mp_r.at[owner],
            device_id=(me, mate), device_id_type=MESH,
        )

    def mix_y(j, origin):
        return pltpu.make_async_remote_copy(
            ms_out.at[y_peer(j)], my_in.at[origin], my_s.at[y_peer(j)], my_r.at[origin],
            device_id=(me, y_peer(j) * 2 + core), device_id_type=MESH,
        )

    def attend(owner):
        start = pl.multiple_of(owner * piece, piece)
        q_rows = q_buf[:, pl.ds(start, piece), :].reshape(heads * piece, LANES)

        def one_block(block, total):
            kv = kv_buf[block]
            logits = lax.dot_general(
                q_rows, kv, (((1,), (1,)), ((), ())), preferred_element_type=F32
            )
            weights = jnp.exp2(logits * factor).astype(BF)
            kv_lane = lax.broadcasted_iota(jnp.int32, kv.shape, 1)
            values = jnp.where(kv_lane < HD, jnp.ones_like(kv), kv)
            return total + jnp.dot(weights, values, preferred_element_type=F32)

        total = lax.fori_loop(0, n_ep, one_block, jnp.zeros((heads * piece, LANES), F32))
        ratio = (total / pltpu.roll(total, HD, 1)).reshape(heads, piece, LANES)
        out_lane = lax.broadcasted_iota(jnp.int32, (piece, LANES), 1)
        tiles = []
        for tile in range(q_ref.shape[1] // LANES):
            left = pltpu.roll(ratio[2 * tile], HD, 1)
            right = ratio[2 * tile + 1] if 2 * tile + 1 < heads else jnp.zeros_like(left)
            tiles.append(jnp.where(out_lane < HD, left, right).astype(BF))
        attended = tiles[0] if len(tiles) == 1 else jnp.concatenate(tiles, axis=1)
        part = jnp.dot(attended, wmix[...], preferred_element_type=F32).astype(BF)
        mp_out[owner] = part.reshape(2, half, part.shape[1])
        mix_mate(owner, 1 - core).start()

    def mix_sum(owner):
        mix_mate(owner, core).wait_recv()
        return mp_out[owner, core].astype(F32) + mp_in[owner].astype(F32)

    loads[3].wait()
    for j in range(1, n_y):
        attend(y_peer(j))
        if j == 1:
            return_rows()
        ms_out[y_peer(j)] = mix_sum(y_peer(j)).astype(BF)
        mix_y(j, my_y).start()
    attend(my_y)

    def ret_wait(o, carry):
        source = (me + n_ep - o) % n_ep
        ret(source, source).wait_recv()
        return carry

    lax.fori_loop(1, n_ep, ret_wait, 0)
    back = ret_in[...].reshape(slots, col_w)
    share = scores_ref[...] / jnp.sum(scores_ref[...], axis=1, keepdims=True)
    rows_a = lax.dot_general(
        pick_a, back, (((0,), (0,)), ((), ())), preferred_element_type=F32
    )
    rows_b = lax.dot_general(
        pick_b, back, (((0,), (0,)), ((), ())), preferred_element_type=F32
    )
    out_ref[...] = (rows_a * share[:, 0:1] + rows_b * share[:, 1:2]).astype(BF)

    total = mix_sum(my_y)
    for j in range(1, n_y):
        mix_y(j, y_peer(j)).wait_recv()
        total = total + my_in[y_peer(j)].astype(F32)
    mixed_ref[...] = total.astype(BF)

    def sends(o, carry):
        peer = (me + o) % n_ep
        disp(peer).wait_send()
        kv_copy(peer, me).wait_send()
        ret(peer, me).wait_send()
        return carry

    lax.fori_loop(1, n_ep, sends, 0)
    for j in range(1, n_y):

        def sent_y(source, carry):
            over_y(j, source, my_y).wait_send()
            return carry

        lax.fori_loop(0, n_ep, sent_y, 0)
        expert_y(j).wait_send()
        mix_y(j, my_y).wait_send()
    for j in range(n_y):
        to_mate(y_peer(j), core).wait_send()
        expert_mate(y_peer(j), 1 - core).wait_send()
        mix_mate(y_peer(j), 1 - core).wait_send()


def local(
    n_ep, n_tp,
    queries, key_input, value_input, query_gain, key_gain, mix_out_weight, expert_input, ffn_gain,
    routes, route_scores, gate_weight, up_weight, down_weight,
):
    rows = queries.shape[0]
    heads = queries.shape[1] // HD
    tp = lax.axis_index("tp")
    n_y = n_tp // 2
    kv_head = tp * heads // (HEADS // KV_HEADS)
    kv = jnp.concatenate(
        [lax.dynamic_slice_in_dim(a, kv_head * HD, HD, 1) for a in (key_input, value_input)], axis=1
    )
    spare = heads % 2 * HD
    if spare:
        queries = jnp.pad(queries, ((0, 0), (0, spare)))
        mix_out_weight = jnp.pad(mix_out_weight, ((0, spare), (0, 0)))
    positions = lax.axis_index("ep") * rows + jnp.arange(rows, dtype=jnp.int32)
    quarter = HD // 4
    lane = jnp.arange(LANES, dtype=jnp.int32)
    inverse = jnp.tile(ROPE_BASE ** (-jnp.arange(quarter, dtype=F32) / quarter), LANES // quarter)
    place = jnp.where(
        (lane % HD < HD // 2)[None, :], (positions // GRID_W)[:, None], (positions % GRID_W)[:, None]
    ).astype(F32)
    angle = place * inverse[None, :]
    cos_table = jnp.cos(angle)
    sin_table = jnp.sin(angle) * jnp.where(lane % (2 * quarter) < quarter, -1.0, 1.0)[None, :]
    width = expert_input.shape[1]
    col_w = width // n_tp
    tokens, top = routes.shape
    own_x = lax.dynamic_slice_in_dim(expert_input, tp * col_w, col_w, 1)
    capacity = 3 * tokens * top // (2 * n_ep)
    slots_per = -(-capacity // 16) * 16
    slots = n_ep * slots_per
    hidden_w = gate_weight.shape[2]
    out_w = mix_out_weight.shape[1]
    half = rows // n_tp
    vm = pltpu.VMEM
    dma = pltpu.SemaphoreType.DMA
    scratch = [
        vm((n_ep, rows, LANES), BF), vm((heads, rows, LANES), BF),
        vm((n_ep, slots_per, col_w), BF), vm((n_tp, n_ep, slots_per, col_w), BF),
        vm((slots, width), BF), vm((slots, hidden_w), BF),
        vm((width, hidden_w), BF), vm((width, hidden_w), BF), vm((hidden_w, width), BF),
        vm(mix_out_weight.shape, BF),
        vm((n_tp, slots, col_w), BF), vm((n_y, slots, col_w), BF), vm((n_y, slots, col_w), BF),
        vm((n_y, slots, col_w), BF),
        vm((n_ep, slots_per, col_w), BF), vm((n_ep, slots_per, col_w), BF),
        vm((n_y, 2, half, out_w), BF), vm((n_y, half, out_w), BF), vm((n_y, half, out_w), BF),
        vm((n_y, half, out_w), BF), vm((8, LANES), F32),
        dma((4,)),
        dma((n_ep,)), dma((n_ep,)), dma((n_ep,)), dma((n_ep,)),
        dma((n_y, n_ep)), dma((n_y, n_ep)),
    ] + [dma((n_y,))] * 6 + [dma((n_ep,))] * 2 + [dma((n_y,))] * 4
    in_vmem = pl.BlockSpec(memory_space=pltpu.VMEM)
    in_any = pl.BlockSpec(memory_space=pl.ANY)
    return pl.pallas_call(
        functools.partial(kernel, n_ep, n_tp, heads, width),
        out_shape=(
            jax.ShapeDtypeStruct((half, out_w), BF),
            jax.ShapeDtypeStruct((tokens, col_w), BF),
        ),
        in_specs=[in_vmem] * 6 + [in_any] + [in_vmem] * 4 + [in_any] * 3,
        out_specs=(in_vmem, in_vmem),
        scratch_shapes=scratch,
        compiler_params=pltpu.CompilerParams(
            collective_id=0, has_side_effects=True, vmem_limit_bytes=60 * 1024 * 1024
        ),
    )(
        queries, kv,
        jnp.tile(query_gain, LANES // HD)[None, :], jnp.tile(key_gain, LANES // HD)[None, :],
        cos_table, sin_table, mix_out_weight, own_x, ffn_gain[None, :], routes.T, route_scores,
        gate_weight, up_weight, down_weight,
    )


def solution(mesh):
    placed = (
        P("ep", "tp"),
        P("ep", None),
        P("ep", None),
        P(),
        P(),
        P("tp", None),
        P("ep", None),
        P(),
        P("ep", None),
        P("ep", None),
        P("ep", None, "tp"),
        P("ep", None, "tp"),
        P("ep", "tp", None),
    )
    return jax.shard_map(
        functools.partial(local, mesh.shape["ep"], mesh.shape["tp"]),
        mesh=mesh,
        in_specs=placed,
        out_specs=(P(("ep", "tp"), None), P("ep", "tp")),
        check_vma=False,
    )
```

```python
import functools
import math

import jax
import jax.numpy as jnp
from jax import lax
from jax.experimental import pallas as pl
from jax.experimental.pallas import tpu as pltpu
from jax.sharding import PartitionSpec as P

HEADS = 16
KV_HEADS = 4
HD = 64
GRID_W = 64
EPSILON = 1e-06
ROPE_BASE = 10000.0
MESH = pl.DeviceIdType.MESH
LANES = 128
BF = jnp.bfloat16
F32 = jnp.float32


def prep(values, gain, cos_table, sin_table):
    width = values.shape[1]
    squares = values * values
    high = squares.astype(BF)
    low = (squares - high.astype(F32)).astype(BF)
    rows = lax.broadcasted_iota(jnp.int32, (width, width), 0) // HD
    cols = lax.broadcasted_iota(jnp.int32, (width, width), 1) // HD
    same = jnp.where(rows == cols, 1.0, 0.0).astype(BF)
    total = jnp.dot(high, same, preferred_element_type=F32) + jnp.dot(
        low, same, preferred_element_type=F32
    )
    gain = jnp.concatenate([gain] * (width // HD), axis=1)
    normed = values * lax.rsqrt(total * (1.0 / HD) + EPSILON) * gain
    lane = lax.broadcasted_iota(jnp.int32, normed.shape, 1)
    quarter = HD // 4
    partner = jnp.where(
        lane % (2 * quarter) < quarter,
        pltpu.roll(normed, width - quarter, 1),
        pltpu.roll(normed, quarter, 1),
    )
    return normed * cos_table + partner * sin_table


def angle_tables(start, rows):
    quarter = HD // 4
    many = rows // GRID_W

    def both(count, first):
        shape = (count, LANES)
        place = lax.broadcasted_iota(jnp.int32, shape, 0) + first
        lane = lax.broadcasted_iota(jnp.int32, shape, 1)
        turn = lane % quarter
        inverse = jnp.zeros(shape, F32)
        for j in range(quarter):
            inverse = jnp.where(turn == j, ROPE_BASE ** (-j / quarter), inverse)
        angle = place.astype(F32) * inverse
        sign = jnp.where(lane % (2 * quarter) < quarter, -1.0, 1.0)
        return jnp.cos(angle), jnp.sin(angle) * sign

    tables = []
    for by_row, by_col in zip(both(max(many, 8), start // GRID_W), both(GRID_W, 0)):
        lane = lax.broadcasted_iota(jnp.int32, by_col.shape, 1)
        tables.append(
            jnp.concatenate(
                [jnp.where(lane % HD < HD // 2, by_row[i:i + 1, :], by_col) for i in range(many)],
                axis=0,
            )
        )
    return tables


def kernel(
    n_ep, n_tp, heads, model_width,
    q_any, k_any, v_any, qg_ref, kg_ref, wmix_ref, x_any, gain_ref, routes_ref,
    scores_ref, wg_ref, wu_ref, wd_ref,
    mixed_ref, out_ref,
    q_ref, k_in, v_in, x_ref, kv_buf, q_buf, x_out, x_buf, scaled, hid, wg, wu, wd, wmix, dp_buf, ep_in, es_buf, ey_in,
    ret_out, ret_in, mp_out, mp_in, ms_out, my_in,
    w_sem, kv_s, kv_r, di_s, di_r, dy_s, dy_r, dc_s, dc_r, ep_s, ep_r, ey_s, ey_r, rt_s, rt_r,
    mp_s, mp_r, my_s, my_r,
):
    n_y = n_tp // 2
    me = lax.axis_index("ep")
    tp = lax.axis_index("tp")
    my_y, core = tp // 2, tp % 2
    mate = my_y * 2 + 1 - core
    rows = q_ref.shape[0]
    kv_head = tp * heads // (HEADS // KV_HEADS)
    kv_tile = pl.ds(pl.multiple_of(kv_head // 2 * LANES, LANES), LANES)
    slots_per = x_buf.shape[2]
    slots = n_ep * slots_per
    col_w = x_buf.shape[3]
    tokens = x_ref.shape[0]
    x_cols = pl.ds(pl.multiple_of(tp * col_w, col_w), col_w)

    def y_peer(j):
        return (my_y + j) % n_y

    loads = [
        pltpu.make_async_copy(src, dst, w_sem.at[i])
        for i, (src, dst) in enumerate(
            (
                (x_any.at[:, x_cols], x_ref),
                (k_any.at[:, kv_tile], k_in),
                (v_any.at[:, kv_tile], v_in),
                (q_any, q_ref),
                (wg_ref.at[0], wg),
                (wu_ref.at[0], wu),
                (wd_ref.at[0], wd),
                (wmix_ref, wmix),
            )
        )
    ]
    for load in loads:
        load.start()

    barrier = pltpu.get_barrier_semaphore()

    def greet(o, carry):
        pl.semaphore_signal(barrier, inc=1, device_id=((me + o) % n_ep, tp), device_id_type=MESH)
        return carry

    lax.fori_loop(1, n_ep, greet, 0)
    for j in range(1, n_y):
        pl.semaphore_signal(
            barrier, inc=1, device_id=(me, y_peer(j) * 2 + core), device_id_type=MESH
        )
    pl.semaphore_signal(barrier, inc=1, device_id=(me, mate), device_id_type=MESH)

    expert_row = lax.broadcasted_iota(jnp.int32, (n_ep, tokens), 0)
    first = jnp.where(expert_row == routes_ref[0:1, :], 1.0, 0.0)
    second = jnp.where(expert_row == routes_ref[1:2, :], 1.0, 0.0)
    earlier = jnp.where(
        lax.broadcasted_iota(jnp.int32, (tokens, tokens), 0)
        < lax.broadcasted_iota(jnp.int32, (tokens, tokens), 1),
        1.0,
        0.0,
    ).astype(BF)
    before = jnp.dot((first + second).astype(BF), earlier, preferred_element_type=F32)
    place = before + expert_row.astype(F32) * slots_per
    slot_a = jnp.sum(first * place, axis=0, keepdims=True).astype(jnp.int32)
    slot_b = jnp.sum(second * place, axis=0, keepdims=True).astype(jnp.int32)
    slot_row = lax.broadcasted_iota(jnp.int32, (slots, tokens), 0)
    pick_a = jnp.where(slot_row == slot_a, 1.0, 0.0).astype(BF)
    pick_b = jnp.where(slot_row == slot_b, 1.0, 0.0).astype(BF)
    loads[0].wait()
    sent = jnp.dot(pick_a + pick_b, x_ref[...], preferred_element_type=F32).astype(BF)
    x_out[...] = sent.reshape(x_out.shape)
    x_buf[tp, me] = x_out[me]

    pl.semaphore_wait(barrier, n_ep - 1 + n_y)

    def disp(peer):
        return pltpu.make_async_remote_copy(
            x_out.at[peer], x_buf.at[tp, me], di_s.at[peer], di_r.at[me],
            device_id=(peer, tp), device_id_type=MESH,
        )

    def disp_in(source):
        return pltpu.make_async_remote_copy(
            x_out.at[source], x_buf.at[tp, source], di_s.at[source], di_r.at[source],
            device_id=(source, tp), device_id_type=MESH,
        )

    n_x = 1 << ((n_ep.bit_length() - 1) // 2)
    n_z = n_ep // n_x
    my_z, my_x = me // n_x, me % n_x

    def z_peer(o):
        return (my_z + o) % n_z * n_x + my_x

    def x_peer(o):
        return my_z * n_x + (my_x + o) % n_x

    def kv_copy(peer, origin, leg):
        return pltpu.make_async_remote_copy(
            kv_buf.at[origin], kv_buf.at[origin], kv_s.at[leg], kv_r.at[origin],
            device_id=(peer, tp), device_id_type=MESH,
        )

    def over_y(j, source, owner):
        return pltpu.make_async_remote_copy(
            x_buf.at[owner * 2 + core, source], x_buf.at[owner * 2 + core, source],
            dy_s.at[y_peer(j), source], dy_r.at[owner, source],
            device_id=(me, y_peer(j) * 2 + core), device_id_type=MESH,
        )

    def start_disp(o, carry):
        disp((me + o) % n_ep).start()
        return carry

    lax.fori_loop(1, n_ep, start_disp, 0)
    for j in range(1, n_y):
        over_y(j, me, my_y).start()

    cos_table, sin_table = angle_tables(me * rows, rows)
    loads[1].wait()
    loads[2].wait()
    odd = kv_head % 2 == 1
    key = k_in[...].astype(F32)
    value = v_in[...].astype(F32)
    key = jnp.where(odd, pltpu.roll(key, HD, 1), key)
    value = jnp.where(odd, value, pltpu.roll(value, HD, 1))
    turned = prep(key, kg_ref[...], cos_table, sin_table)
    lane = lax.broadcasted_iota(jnp.int32, key.shape, 1)
    kv_buf[me] = jnp.where(lane < HD, turned, value).astype(BF)

    loads[3].wait()
    for tile in range(q_ref.shape[1] // LANES):
        q_tile = prep(
            q_ref[:, tile * LANES:(tile + 1) * LANES].astype(F32),
            qg_ref[...], cos_table, sin_table,
        )
        q_lane = lax.broadcasted_iota(jnp.int32, q_tile.shape, 1)
        for part in range(2):
            head = tile * 2 + part
            if head < heads:
                moved = q_tile if part == 0 else pltpu.roll(q_tile, HD, 1)
                q_buf[head] = jnp.where(q_lane < HD, moved, 0.0).astype(BF)

    def forward(o, carry):
        source = (me + n_ep - o) % n_ep
        disp_in(source).wait_recv()
        for j in range(1, n_y):
            over_y(j, source, my_y).start()
        return carry

    lax.fori_loop(1, n_ep, forward, 0)
    for o in range(1, n_x):
        kv_copy(x_peer(o), me, o).start()
    for o in range(1, n_z):
        kv_copy(z_peer(o), me, o * n_x).start()

    def to_mate(owner, mine):
        quarter = owner * 2 + mine
        return pltpu.make_async_remote_copy(
            x_buf.at[quarter], x_buf.at[quarter], dc_s.at[owner], dc_r.at[owner],
            device_id=(me, mate), device_id_type=MESH,
        )

    to_mate(my_y, core).start()
    for j in range(1, n_y):
        owner = y_peer(j)

        def arrived(source, carry):
            over_y(j, source, owner).wait_recv()
            return carry

        lax.fori_loop(0, n_ep, arrived, 0)
        to_mate(owner, core).start()
    for j in range(n_y):
        to_mate(y_peer(j), 1 - core).wait_recv()

    power = jnp.zeros((slots, 1), F32)
    for q in range(n_tp):
        x_q = x_buf[q].reshape(slots, col_w).astype(F32)
        power = power + jnp.sum(x_q * x_q, axis=1, keepdims=True)
        scaled[:, q * col_w:(q + 1) * col_w] = (
            x_q * gain_ref[:, q * col_w:(q + 1) * col_w]
        ).astype(BF)
    row_scale = lax.rsqrt(power * (1.0 / model_width) + EPSILON)
    loads[4].wait()
    loads[5].wait()
    hidden_w = wg.shape[1]
    tile_w = math.gcd(hidden_w, 256)

    def hidden_tile(i, carry):
        cols = pl.ds(pl.multiple_of(i * tile_w, tile_w), tile_w)
        gate = row_scale * jnp.dot(scaled[...], wg[:, cols], preferred_element_type=F32)
        up = row_scale * jnp.dot(scaled[...], wu[:, cols], preferred_element_type=F32)
        hid[:, cols] = (gate / (1.0 + jnp.exp(-gate)) * up).astype(BF)
        return carry

    lax.fori_loop(0, hidden_w // tile_w, hidden_tile, 0)
    loads[6].wait()
    for q in range(n_tp):
        dp_buf[q] = jnp.dot(
            hid[...], wd[:, q * col_w:(q + 1) * col_w], preferred_element_type=F32
        ).astype(BF)

    for o in range(1, n_z):
        origin = z_peer(n_z - o)
        kv_copy(origin, origin, 0).wait_recv()
        for i in range(1, n_x):
            kv_copy(x_peer(i), origin, o * n_x + i).start()

    def expert_mate(owner, side):
        return pltpu.make_async_remote_copy(
            dp_buf.at[owner * 2 + side], ep_in.at[owner], ep_s.at[owner], ep_r.at[owner],
            device_id=(me, mate), device_id_type=MESH,
        )

    def expert_y(j):
        return pltpu.make_async_remote_copy(
            es_buf.at[y_peer(j)], ey_in.at[my_y], ey_s.at[y_peer(j)], ey_r.at[my_y],
            device_id=(me, y_peer(j) * 2 + core), device_id_type=MESH,
        )

    def expert_y_in(j):
        return pltpu.make_async_remote_copy(
            es_buf.at[y_peer(j)], ey_in.at[y_peer(j)], ey_s.at[y_peer(j)], ey_r.at[y_peer(j)],
            device_id=(me, y_peer(j) * 2 + core), device_id_type=MESH,
        )

    for j in range(n_y):
        expert_mate(y_peer((j + 1) % n_y), 1 - core).start()

    def mate_sum(j):
        owner = y_peer(j)
        expert_mate(owner, core).wait_recv()
        return dp_buf[owner * 2 + core].astype(F32) + ep_in[owner].astype(F32)

    for j in range(1, n_y):
        es_buf[y_peer(j)] = mate_sum(j).astype(BF)
        expert_y(j).start()

    def ret(peer, origin):
        return pltpu.make_async_remote_copy(
            ret_out.at[peer], ret_in.at[origin], rt_s.at[peer], rt_r.at[origin],
            device_id=(peer, tp), device_id_type=MESH,
        )

    def return_rows():
        total = mate_sum(0)
        for j in range(1, n_y):
            expert_y_in(j).wait_recv()
            total = total + ey_in[y_peer(j)].astype(F32)
        ret_out[...] = total.astype(BF).reshape(ret_out.shape)
        ret_in[me] = ret_out[me]

        def start_ret(o, carry):
            ret((me + o) % n_ep, me).start()
            return carry

        lax.fori_loop(1, n_ep, start_ret, 0)

    piece = rows // n_y
    half = piece // 2
    factor = HD ** (-0.5) * math.log2(math.e)

    def mix_mate(owner, side):
        return pltpu.make_async_remote_copy(
            mp_out.at[owner, side], mp_in.at[owner], mp_s.at[owner], mp_r.at[owner],
            device_id=(me, mate), device_id_type=MESH,
        )

    def mix_y(j, origin):
        return pltpu.make_async_remote_copy(
            ms_out.at[y_peer(j)], my_in.at[origin], my_s.at[y_peer(j)], my_r.at[origin],
            device_id=(me, y_peer(j) * 2 + core), device_id_type=MESH,
        )

    def attend(owner):
        start = pl.multiple_of(owner * piece, piece)
        q_rows = q_buf[:, pl.ds(start, piece), :].reshape(heads * piece, LANES)

        def one_block(block, total):
            kv = kv_buf[block]
            logits = lax.dot_general(
                q_rows, kv, (((1,), (1,)), ((), ())), preferred_element_type=F32
            )
            weights = jnp.exp2(logits * factor).astype(BF)
            kv_lane = lax.broadcasted_iota(jnp.int32, kv.shape, 1)
            values = jnp.where(kv_lane < HD, jnp.ones_like(kv), kv)
            return total + jnp.dot(weights, values, preferred_element_type=F32)

        total = lax.fori_loop(0, n_ep, one_block, jnp.zeros((heads * piece, LANES), F32))
        ratio = (total / pltpu.roll(total, HD, 1)).reshape(heads, piece, LANES)
        out_lane = lax.broadcasted_iota(jnp.int32, (piece, LANES), 1)
        tiles = []
        for tile in range(q_ref.shape[1] // LANES):
            left = pltpu.roll(ratio[2 * tile], HD, 1)
            right = ratio[2 * tile + 1] if 2 * tile + 1 < heads else jnp.zeros_like(left)
            tiles.append(jnp.where(out_lane < HD, left, right).astype(BF))
        attended = tiles[0] if len(tiles) == 1 else jnp.concatenate(tiles, axis=1)
        part = jnp.dot(attended, wmix[...], preferred_element_type=F32).astype(BF)
        mp_out[owner] = part.reshape(2, half, part.shape[1])
        mix_mate(owner, 1 - core).start()

    def mix_sum(owner):
        mix_mate(owner, core).wait_recv()
        return mp_out[owner, core].astype(F32) + mp_in[owner].astype(F32)

    for o in range(n_z):
        for i in range(1, n_x):
            origin = (my_z + n_z - o) % n_z * n_x + (my_x + n_x - i) % n_x
            kv_copy(x_peer(i), origin, 0).wait_recv()
    loads[7].wait()
    for j in range(1, n_y):
        attend(y_peer(j))
        if j == 1:
            return_rows()
        ms_out[y_peer(j)] = mix_sum(y_peer(j)).astype(BF)
        mix_y(j, my_y).start()
    attend(my_y)

    def ret_wait(o, carry):
        source = (me + n_ep - o) % n_ep
        ret(source, source).wait_recv()
        return carry

    lax.fori_loop(1, n_ep, ret_wait, 0)
    back = ret_in[...].reshape(slots, col_w)
    share_row = scores_ref[...] / jnp.sum(scores_ref[...], axis=0, keepdims=True)
    own_token = lax.broadcasted_iota(jnp.int32, (tokens, tokens), 0) == lax.broadcasted_iota(
        jnp.int32, (tokens, tokens), 1
    )
    share_a, share_b = (
        jnp.sum(jnp.where(own_token, share_row[i:i + 1, :], 0.0), axis=1, keepdims=True)
        for i in range(2)
    )
    rows_a = lax.dot_general(
        pick_a, back, (((0,), (0,)), ((), ())), preferred_element_type=F32
    )
    rows_b = lax.dot_general(
        pick_b, back, (((0,), (0,)), ((), ())), preferred_element_type=F32
    )
    out_ref[...] = (rows_a * share_a + rows_b * share_b).astype(BF)

    total = mix_sum(my_y)
    for j in range(1, n_y):
        mix_y(j, y_peer(j)).wait_recv()
        total = total + my_in[y_peer(j)].astype(F32)
    mixed_ref[...] = total.astype(BF)

    def sends(o, carry):
        peer = (me + o) % n_ep
        disp(peer).wait_send()
        kv_copy(peer, me, o).wait_send()
        ret(peer, me).wait_send()
        return carry

    lax.fori_loop(1, n_ep, sends, 0)
    for j in range(1, n_y):

        def sent_y(source, carry):
            over_y(j, source, my_y).wait_send()
            return carry

        lax.fori_loop(0, n_ep, sent_y, 0)
        expert_y(j).wait_send()
        mix_y(j, my_y).wait_send()
    for j in range(n_y):
        to_mate(y_peer(j), core).wait_send()
        expert_mate(y_peer(j), 1 - core).wait_send()
        mix_mate(y_peer(j), 1 - core).wait_send()


def local(
    n_ep, n_tp,
    queries, key_input, value_input, query_gain, key_gain, mix_out_weight, expert_input, ffn_gain,
    routes, route_scores, gate_weight, up_weight, down_weight,
):
    rows = queries.shape[0]
    heads = queries.shape[1] // HD
    n_y = n_tp // 2
    spare = heads % 2 * HD
    if spare:
        queries = jnp.pad(queries, ((0, 0), (0, spare)))
        mix_out_weight = jnp.pad(mix_out_weight, ((0, spare), (0, 0)))
    width = expert_input.shape[1]
    col_w = width // n_tp
    tokens, top = routes.shape
    capacity = 3 * tokens * top // (2 * n_ep)
    slots_per = -(-capacity // 16) * 16
    slots = n_ep * slots_per
    hidden_w = gate_weight.shape[2]
    out_w = mix_out_weight.shape[1]
    half = rows // n_tp
    vm = pltpu.VMEM
    dma = pltpu.SemaphoreType.DMA
    scratch = [
        vm(queries.shape, BF), vm((rows, LANES), BF), vm((rows, LANES), BF), vm((tokens, col_w), BF),
        vm((n_ep, rows, LANES), BF), vm((heads, rows, LANES), BF),
        vm((n_ep, slots_per, col_w), BF), vm((n_tp, n_ep, slots_per, col_w), BF),
        vm((slots, width), BF), vm((slots, hidden_w), BF),
        vm((width, hidden_w), BF), vm((width, hidden_w), BF), vm((hidden_w, width), BF),
        vm(mix_out_weight.shape, BF),
        vm((n_tp, slots, col_w), BF), vm((n_y, slots, col_w), BF), vm((n_y, slots, col_w), BF),
        vm((n_y, slots, col_w), BF),
        vm((n_ep, slots_per, col_w), BF), vm((n_ep, slots_per, col_w), BF),
        vm((n_y, 2, half, out_w), BF), vm((n_y, half, out_w), BF), vm((n_y, half, out_w), BF),
        vm((n_y, half, out_w), BF),
        dma((8,)),
        dma((n_ep,)), dma((n_ep,)), dma((n_ep,)), dma((n_ep,)),
        dma((n_y, n_ep)), dma((n_y, n_ep)),
    ] + [dma((n_y,))] * 6 + [dma((n_ep,))] * 2 + [dma((n_y,))] * 4
    in_vmem = pl.BlockSpec(memory_space=pltpu.VMEM)
    in_any = pl.BlockSpec(memory_space=pl.ANY)
    return pl.pallas_call(
        functools.partial(kernel, n_ep, n_tp, heads, width),
        out_shape=(
            jax.ShapeDtypeStruct((half, out_w), BF),
            jax.ShapeDtypeStruct((tokens, col_w), BF),
        ),
        in_specs=[in_any] * 3 + [in_vmem] * 2 + [in_any] * 2 + [in_vmem] * 3 + [in_any] * 3,
        out_specs=(in_vmem, in_vmem),
        scratch_shapes=scratch,
        compiler_params=pltpu.CompilerParams(
            collective_id=0, has_side_effects=True, vmem_limit_bytes=60 * 1024 * 1024
        ),
    )(
        queries, key_input, value_input, query_gain[None, :], key_gain[None, :],
        mix_out_weight, expert_input, ffn_gain[None, :], routes.T, route_scores.T,
        gate_weight, up_weight, down_weight,
    )


def solution(mesh):
    placed = (
        P("ep", "tp"),
        P("ep", None),
        P("ep", None),
        P(),
        P(),
        P("tp", None),
        P("ep", None),
        P(),
        P("ep", None),
        P("ep", None),
        P("ep", None, "tp"),
        P("ep", None, "tp"),
        P("ep", "tp", None),
    )
    return jax.shard_map(
        functools.partial(local, mesh.shape["ep"], mesh.shape["tp"]),
        mesh=mesh,
        in_specs=placed,
        out_specs=(P(("ep", "tp"), None), P("ep", "tp")),
        check_vma=False,
    )
```
